32 devices in a mesh: sp: 16 (over z, y, x), tp: 2 (over core).
Axes of the slice: x: 2, y: 2, z: 4, core: 2. Of those that a mesh axis runs over, the one named last changes fastest.
Arguments:
- tokens: bfloat16 [4096, 2048], P(('sp', 'tp')), may hold values from -6 to 6
- gain: float32 [2048], replicated, may hold values from 0.1 to 1.9
- w_ret_q: bfloat16 [2048, 2048], P(None, 'tp'), may hold values from -0.125 to 0.125
- w_ret_k: bfloat16 [2048, 2048], P(None, 'tp'), may hold values from -0.125 to 0.125
- w_ret_v: bfloat16 [2048, 2048], P(None, 'tp'), may hold values from -0.125 to 0.125
- w_fox_q: bfloat16 [2048, 1024], P(None, 'tp'), may hold values from -0.125 to 0.125
- w_fox_k: bfloat16 [2048, 1024], P(None, 'tp'), may hold values from -0.125 to 0.125
- w_fox_v: bfloat16 [2048, 1024], P(None, 'tp'), may hold values from -0.125 to 0.125
- fox_gates: float32 [4096, 8], P('sp', 'tp'), may hold values from -4096 to 0, as said below
- w_out_ret: bfloat16 [2048, 2048], P('tp', 'sp'), may hold values from -0.109375 to 0.109375
- w_out_fox: bfloat16 [1024, 2048], P('tp', 'sp'), may hold values from -0.109375 to 0.109375
Outputs:
- mixed: bfloat16 [4096, 2048], P(('sp', 'tp'))
The draws below stay inside these ranges and needn't reach their ends.
Inputs may be any that keep to these rules, and one draw needn't show every extreme that they name: `fox_gates`: each head's values never rise along positions.
All inputs are finite; a program needn't handle non-finite values.
Results may differ from the reference program's by a relative error of at most 0.02.
Values may be sent and summed in bfloat16 or wider, within the bound.
A program may use at most 128 MiB of HBM per device.

```python
import math
import jax
import jax.numpy as jnp
from jax import lax

D = 2048
RET_HEADS = 8
RET_DIM = 256
FORGET_HEADS = 8
FOX_DIM = 128
BLOCK = 128
TOK_DEV = 256
SEQUENCE_TOKENS = 4096
N_TP = 2


def draw_fox_gates(key, part):
    ranking = jax.random.permutation(jax.random.fold_in(key, 11), FORGET_HEADS)
    slow_heads = ranking < FORGET_HEADS // 2
    roughness = jax.random.uniform(jax.random.fold_in(key, 14), (SEQUENCE_TOKENS, FORGET_HEADS), jnp.float32, 0.5, 1.5)
    fast_rate = 1.0 / jax.random.uniform(jax.random.fold_in(key, 12), (FORGET_HEADS,), jnp.float32, 30.0, 50.0)
    slow_rate = jax.random.uniform(jax.random.fold_in(key, 13), (FORGET_HEADS,), jnp.float32, 0.1, 0.4) / SEQUENCE_TOKENS
    base_rate = jnp.where(slow_heads, slow_rate, fast_rate)
    block_count = SEQUENCE_TOKENS // TOK_DEV
    block_factor = jnp.exp(jax.random.uniform(jax.random.fold_in(key, 15), (block_count, FORGET_HEADS), jnp.float32, 0.0, math.log(4.0)))
    block_factor = jnp.repeat(block_factor, TOK_DEV, axis=0)
    forget_strength = base_rate[None, :] * roughness * block_factor
    spike_locations = jax.random.randint(jax.random.fold_in(key, 16), (2, FORGET_HEADS), 0, SEQUENCE_TOKENS)
    token_positions = jnp.arange(SEQUENCE_TOKENS, dtype=jnp.int32)
    spike_mask = jnp.any(token_positions[None, :, None] == spike_locations[:, None, :], axis=0)
    retain_fraction = jax.random.uniform(jax.random.fold_in(key, 17), (SEQUENCE_TOKENS, FORGET_HEADS), jnp.float32, 0.5, 0.8)
    forget_strength = forget_strength + jnp.where(spike_mask, -jnp.log(retain_fraction), 0.0)
    return -jnp.cumsum(forget_strength, axis=0)


def block_scale(key, dims, pieces, smallest, high):
    factor_of, own = 1.0, jax.random.fold_in(key, 6)
    for position, parts in pieces:
        draws = jnp.exp(jax.random.uniform(jax.random.fold_in(own, position), (parts,), jnp.float32, smallest / len(pieces), high / len(pieces)))
        factor_of = factor_of * jnp.repeat(draws, dims[position] // parts).reshape([-1 if axis == position else 1 for axis in range(len(dims))])
    return factor_of


def bell_draw(rng, dims, scale, limit, split=(), kind=jnp.bfloat16):
    result = scale * jax.random.normal(rng, dims, jnp.float32)
    if split:
        result = result * block_scale(rng, dims, split, -0.22, 0.18)
    return jnp.clip(result, -limit, limit).astype(kind)


def setup_inputs(seed: int = 0) -> dict:
    splits = jax.random.split(jax.random.key(seed), 12)
    return {
        "tokens": bell_draw(splits[0], (SEQUENCE_TOKENS, D), 1.0, 6.0, ((0, 32),)),
        "gain": jnp.clip(1.0 + 0.18 * jax.random.normal(splits[1], (D,), jnp.float32), 0.1, 1.9),
        "w_ret_q": bell_draw(splits[2], (D, RET_HEADS * RET_DIM), D ** -0.5, 0.125, ((1, 2),)),
        "w_ret_k": bell_draw(splits[3], (D, RET_HEADS * RET_DIM), D ** -0.5, 0.125, ((1, 2),)),
        "w_ret_v": bell_draw(splits[4], (D, RET_HEADS * RET_DIM), D ** -0.5, 0.125, ((1, 2),)),
        "w_fox_q": bell_draw(splits[5], (D, FORGET_HEADS * FOX_DIM), D ** -0.5, 0.125, ((1, 2),)),
        "w_fox_k": bell_draw(splits[6], (D, FORGET_HEADS * FOX_DIM), D ** -0.5, 0.125, ((1, 2),)),
        "w_fox_v": bell_draw(splits[7], (D, FORGET_HEADS * FOX_DIM), D ** -0.5, 0.125, ((1, 2),)),
        "fox_gates": draw_fox_gates(jax.random.fold_in(splits[11], 71), 0),
        "w_out_ret": bell_draw(splits[9], (RET_HEADS * RET_DIM, D), (RET_HEADS * RET_DIM + FORGET_HEADS * FOX_DIM) ** -0.5, 0.109375, ((0, 2), (1, 16))),
        "w_out_fox": bell_draw(splits[10], (FORGET_HEADS * FOX_DIM, D), (RET_HEADS * RET_DIM + FORGET_HEADS * FOX_DIM) ** -0.5, 0.109375, ((0, 2), (1, 16))),
    }


eps = 1e-06

def to_half(values):
    return lax.optimization_barrier(values.astype(jnp.bfloat16))

def head_norm(values, width):
    rows_here = values.shape[0]
    grouped = values.reshape(rows_here, -1, width)
    scaled = grouped * lax.rsqrt(lax.optimization_barrier(jnp.mean(grouped * grouped, axis=2, keepdims=True)) + eps)
    return scaled.reshape(rows_here, -1).astype(jnp.bfloat16)

def rotate(values, token_positions, width):
    rows_here = values.shape[0]
    half_width = width // 2
    inverse = 10000.0 ** (-jnp.arange(half_width, dtype=jnp.float32) / half_width)
    angles = token_positions.astype(jnp.float32)[:, None] * inverse[None, :]
    cosine = jnp.cos(angles)[:, None, :]
    sine = jnp.sin(angles)[:, None, :]
    grouped = values.astype(jnp.float32).reshape(rows_here, -1, width)
    first_half = grouped[..., :half_width]
    second_half = grouped[..., half_width:]
    turned = jnp.concatenate([first_half * cosine - second_half * sine, first_half * sine + second_half * cosine], axis=-1)
    return turned.reshape(rows_here, -1)

def decay_rates(head_ids, total):
    heads_float = head_ids.astype(jnp.float32)
    middle = RET_HEADS // 2
    fast_rate = 1.0 / (32.0 + 16.0 * heads_float)
    slow_rate = jnp.exp2(-(heads_float - middle)) / total
    return jnp.where(head_ids < middle, fast_rate, slow_rate)

def decay_tables(rates):
    offsets = jnp.arange(BLOCK, dtype=jnp.float32)
    spread = offsets[:, None] - offsets[None, :]
    causal = spread >= 0
    within = jnp.where(causal[None], jnp.exp(-rates[:, None, None] * jnp.where(causal, spread, 0.0)[None]), 0.0)
    query_decay = jnp.exp(-rates[None, :] * (offsets[:, None] + 1.0))
    key_decay = jnp.exp(-rates[None, :] * (BLOCK - 1.0 - offsets[:, None]))
    block_decay = jnp.exp(-rates * BLOCK)
    return (within, query_decay, key_decay, block_decay)

def retention(queries, keys, values, rates):
    heads = RET_HEADS
    within, query_decay, key_decay, block_decay = decay_tables(rates)
    count = queries.shape[0] // BLOCK

    def shaped(array):
        return array.astype(jnp.float32).reshape(count, BLOCK, heads, RET_DIM)

    def step(carry, blocks):
        query_block, key_block, value_block = blocks
        scores = jnp.einsum('thd,shd->hts', query_block, key_block, precision=lax.Precision.HIGHEST) * within
        inner = jnp.einsum('hts,she->the', to_half(scores).astype(jnp.float32), value_block, precision=lax.Precision.HIGHEST)
        cross = jnp.einsum('thd,hde->the', query_block, carry, precision=lax.Precision.HIGHEST) * query_decay[:, :, None]
        scaled = to_half(key_block * key_decay[:, :, None]).astype(jnp.float32)
        new_state = carry * block_decay[:, None, None] + jnp.einsum('shd,she->hde', scaled, value_block, precision=lax.Precision.HIGHEST)
        return (new_state, inner + cross)
    start_state = jnp.zeros((heads, RET_DIM, RET_DIM), jnp.float32)
    _, outputs = lax.scan(step, start_state, (shaped(queries), shaped(keys), shaped(values)))
    return outputs.reshape(count * BLOCK, heads * RET_DIM)

def forgetting(queries, keys, values, gates):
    total = queries.shape[0]
    heads = FORGET_HEADS
    width = math.gcd(total, 512)
    query3 = queries.astype(jnp.float32).reshape(total, heads, FOX_DIM)
    key3 = keys.astype(jnp.float32).reshape(total, heads, FOX_DIM)
    value3 = values.astype(jnp.float32).reshape(total, heads, FOX_DIM)
    key_pos = jnp.arange(total, dtype=jnp.int32)

    def one_block(index):
        begin = (index * width).astype(jnp.int32)
        block = lax.dynamic_slice_in_dim(query3, begin, width, 0)
        query_gates = lax.dynamic_slice_in_dim(gates, begin, width, 0)
        scores = jnp.einsum('qhd,khd->hqk', block, key3, precision=lax.Precision.HIGHEST) * FOX_DIM ** (-0.5)
        scores = scores + query_gates.T[:, :, None] - gates.T[:, None, :]
        query_pos = begin + jnp.arange(width, dtype=jnp.int32)
        allowed = key_pos[None, :] <= query_pos[:, None]
        weights = jnp.exp(jnp.where(allowed[None], scores, -jnp.inf))
        denom = lax.optimization_barrier(jnp.sum(weights, axis=2))
        numer = jnp.einsum('hqk,khd->qhd', to_half(weights).astype(jnp.float32), value3, precision=lax.Precision.HIGHEST)
        return numer / denom.T[:, :, None]
    outputs = lax.map(one_block, jnp.arange(total // width, dtype=jnp.int32))
    return outputs.reshape(total, heads * FOX_DIM)

def reference(tokens, gain, w_ret_q, w_ret_k, w_ret_v, w_fox_q, w_fox_k, w_fox_v, fox_gates, w_out_ret, w_out_fox):
    inputs = tokens.astype(jnp.float32)
    normed = (inputs * lax.rsqrt(lax.optimization_barrier(jnp.mean(inputs * inputs, axis=1, keepdims=True)) + eps) * gain).astype(jnp.bfloat16)
    ret_query = to_half(jnp.dot(normed, w_ret_q, preferred_element_type=jnp.float32))
    ret_key = to_half(jnp.dot(normed, w_ret_k, preferred_element_type=jnp.float32))
    ret_value = to_half(jnp.dot(normed, w_ret_v, preferred_element_type=jnp.float32))
    fox_query = to_half(jnp.dot(normed, w_fox_q, preferred_element_type=jnp.float32))
    fox_key = to_half(jnp.dot(normed, w_fox_k, preferred_element_type=jnp.float32))
    fox_value = to_half(jnp.dot(normed, w_fox_v, preferred_element_type=jnp.float32))
    token_positions = jnp.arange(SEQUENCE_TOKENS, dtype=jnp.int32)
    query_rot = to_half(rotate(ret_query, token_positions, RET_DIM))
    key_rot = to_half(rotate(ret_key, token_positions, RET_DIM) * RET_DIM ** (-0.5))
    rates = decay_rates(jnp.arange(RET_HEADS, dtype=jnp.int32), float(SEQUENCE_TOKENS))
    ret_mixed = head_norm(retention(query_rot, key_rot, ret_value, rates), RET_DIM)
    fox_mixed = head_norm(forgetting(fox_query, fox_key, fox_value, fox_gates), FOX_DIM)
    ret_run = ret_mixed.shape[1] // N_TP
    fox_run = fox_mixed.shape[1] // N_TP

    def group(total, index):
        ret_rows = lax.dynamic_slice_in_dim(ret_mixed, index * ret_run, ret_run, 1)
        ret_weight = lax.dynamic_slice_in_dim(w_out_ret, index * ret_run, ret_run, 0)
        fox_rows = lax.dynamic_slice_in_dim(fox_mixed, index * fox_run, fox_run, 1)
        fox_weight = lax.dynamic_slice_in_dim(w_out_fox, index * fox_run, fox_run, 0)
        partial_sum = jnp.dot(ret_rows, ret_weight, preferred_element_type=jnp.float32) + jnp.dot(fox_rows, fox_weight, preferred_element_type=jnp.float32)
        return (total + to_half(partial_sum).astype(jnp.float32), None)
    summed, _ = lax.scan(group, jnp.zeros((SEQUENCE_TOKENS, D), jnp.float32), jnp.arange(N_TP, dtype=jnp.int32))
    return summed.astype(jnp.bfloat16)
```

```python
import functools
import math

import jax
import jax.numpy as jnp
from jax import lax
from jax.experimental import pallas as pl
from jax.experimental.pallas import tpu as pltpu
from jax.sharding import PartitionSpec as P

RET_HEADS = 8
RET_DIM = 256
FOX_DIM = 128
BLOCK = 128
MESH = pl.DeviceIdType.MESH
VMEM_LIMIT = 60 * 1024 * 1024

eps = 1e-06


def remote(src, dst, send, recv, sp, tp):
    return pltpu.make_async_remote_copy(
        src_ref=src,
        dst_ref=dst,
        send_sem=send,
        recv_sem=recv,
        device_id=(sp, tp),
        device_id_type=MESH,
    )


def gather_kernel(
    n_sp,
    n_tp,
    group,
    tok_ref,
    gain_ref,
    gates_ref,
    wr_ref,
    wf_ref,
    xall,
    gall,
    wz,
    own,
    local_sem,
    tsend,
    trecv,
    dsend,
    drecv,
    psend,
    precv,
    gsend,
    grecv,
    usend,
    urecv,
    nsend,
    nrecv,
):
    sp = lax.axis_index("sp")
    tp = lax.axis_index("tp")
    g = lax.rem(sp, group)
    z = sp // group
    depth = n_sp // group
    rows = tok_ref.shape[0]
    half = rows // 2
    krows = wr_ref.shape[0]

    barrier = pltpu.get_barrier_semaphore()
    for i in range(1, n_sp):
        pl.semaphore_signal(
            barrier, inc=1, device_id=(lax.rem(sp + i, n_sp), tp), device_id_type=MESH
        )
    for i in range(1, n_tp):
        pl.semaphore_signal(
            barrier, inc=1, device_id=(sp, lax.rem(tp + i, n_tp)), device_id_type=MESH
        )

    values = tok_ref[...].astype(jnp.float32)
    scale = lax.rsqrt(jnp.mean(values * values, axis=1, keepdims=True) + eps)
    own[...] = (values * scale * gain_ref[...]).astype(jnp.bfloat16)
    copies = [
        pltpu.make_async_copy(wr_ref, wz.at[z, pl.ds(0, krows)], local_sem.at[0]),
        pltpu.make_async_copy(
            wf_ref, wz.at[z, pl.ds(krows, wf_ref.shape[0])], local_sem.at[1]
        ),
        pltpu.make_async_copy(gates_ref, gall.at[sp], local_sem.at[2]),
    ]
    for copy in copies:
        copy.start()
    pl.semaphore_wait(barrier, n_sp + n_tp - 2)

    def slot(which, core):
        return xall.at[which * n_tp + core]

    mine = pltpu.make_async_copy(own, slot(g, tp), local_sem.at[3])
    mine.start()

    def peer(other):
        return z * group + other

    hyper = group == 4
    direct = []
    for i in range(1, group):
        if hyper and i == 3:
            continue
        other = lax.bitwise_xor(g, i) if hyper else lax.rem(g + i, group)
        direct.append(
            remote(own, slot(g, tp), tsend.at[i], trecv.at[i], peer(other), tp)
        )
    for copy in direct:
        copy.start()
    pair = []
    for i in range(1, n_tp):
        copy = remote(
            own, slot(g, tp), psend.at[0, i], precv.at[0, i], sp, lax.rem(tp + i, n_tp)
        )
        copy.start()
        pair.append(copy)
    gate_copies = []
    for i in range(1, n_sp):
        copy = remote(
            gates_ref, gall.at[sp], gsend.at[i], grecv.at[i], lax.rem(sp + i, n_sp), tp
        )
        copy.start()
        gate_copies.append(copy)

    copies[0].wait()
    copies[1].wait()

    def up(block):
        return remote(
            wz.at[block],
            wz.at[block],
            usend.at[block],
            urecv.at[block],
            lax.rem(sp + group, n_sp),
            tp,
        )

    def down(block):
        return remote(
            wz.at[block],
            wz.at[block],
            nsend.at[block],
            nrecv.at[block],
            lax.rem(sp + n_sp - group, n_sp),
            tp,
        )

    @pl.when(z < depth - 1)
    def _():
        up(z).start()

    @pl.when(z > 0)
    def _():
        down(z).start()

    def forward(which, row):
        for i in range(1, n_tp):
            copy = remote(
                slot(which, tp),
                slot(which, tp),
                psend.at[row, i],
                precv.at[row, i],
                sp,
                lax.rem(tp + i, n_tp),
            )
            copy.start()
            pair.append(copy)

    if hyper:
        relays = []
        for i in (1, 2):
            direct[i - 1].wait_recv()
            source = lax.bitwise_xor(g, i)
            target = lax.bitwise_xor(g, 3 - i)
            part = pl.ds((i - 1) * half, half)
            copy = remote(
                slot(source, tp).at[part],
                slot(source, tp).at[part],
                dsend.at[i],
                drecv.at[i],
                peer(target),
                tp,
            )
            copy.start()
            relays.append(copy)
            forward(source, i)
    else:
        for i in range(1, group):
            direct[i - 1].wait_recv()
            forward(lax.rem(g + group - i, group), i)

    def line(step, carry):
        below = z - step
        above = z + step

        @pl.when(below >= 0)
        def _():
            up(below).wait_recv()

            @pl.when(z < depth - 1)
            def _():
                up(below).start()

        @pl.when(above <= depth - 1)
        def _():
            down(above).wait_recv()

            @pl.when(z > 0)
            def _():
                down(above).start()

        return carry

    split = depth // 2 if hyper else depth
    lax.fori_loop(1, split, line, 0)
    if hyper:
        for copy in relays:
            copy.wait_recv()
        forward(lax.bitwise_xor(g, 3), 3)
    lax.fori_loop(split, depth, line, 0)

    def settle(step, carry):
        @pl.when((z < depth - 1) & (step <= z))
        def _():
            up(step).wait_send()

        @pl.when((z > 0) & (step >= z))
        def _():
            down(step).wait_send()

        return carry

    lax.fori_loop(0, depth, settle, 0)
    for copy in direct:
        copy.wait_send()
    if hyper:
        for copy in relays:
            copy.wait_send()
    for copy in gate_copies + pair:
        copy.wait()
    copies[2].wait()
    mine.wait()


def gather(tokens, gain, gates, w_ret, w_fox, n_sp, n_tp, group):
    rows, width = tokens.shape
    depth = n_sp // group
    out_rows = w_ret.shape[0] + w_fox.shape[0]
    vmem = pl.BlockSpec(memory_space=pltpu.VMEM)
    hbm = pl.BlockSpec(memory_space=pl.ANY)
    dma = pltpu.SemaphoreType.DMA
    return pl.pallas_call(
        functools.partial(gather_kernel, n_sp, n_tp, group),
        out_shape=(
            jax.ShapeDtypeStruct((group * n_tp, rows, width), jnp.bfloat16),
            jax.ShapeDtypeStruct((n_sp,) + gates.shape, jnp.float32),
            jax.ShapeDtypeStruct((depth, out_rows, w_ret.shape[1]), jnp.bfloat16),
        ),
        in_specs=[vmem, vmem, vmem, hbm, hbm],
        out_specs=(hbm, vmem, hbm),
        scratch_shapes=[
            pltpu.VMEM((rows, width), jnp.bfloat16),
            dma((4,)),
            dma((max(group, 2),)),
            dma((max(group, 2),)),
            dma((3,)),
            dma((3,)),
            dma((group, n_tp)),
            dma((group, n_tp)),
            dma((n_sp,)),
            dma((n_sp,)),
            dma((depth,)),
            dma((depth,)),
            dma((depth,)),
            dma((depth,)),
        ],
        compiler_params=pltpu.CompilerParams(
            collective_id=0, has_side_effects=True, vmem_limit_bytes=VMEM_LIMIT
        ),
        name="gather",
    )(tokens, gain, gates, w_ret, w_fox)


def normalize(values):
    return (
        values * lax.rsqrt(jnp.mean(values * values, axis=1, keepdims=True) + eps)
    ).astype(jnp.bfloat16)


def mixer_kernel(
    n_sp,
    n_tp,
    group,
    rq,
    rk,
    rv,
    fq,
    fkv,
    gq,
    gk,
    within,
    qdec,
    kdec,
    bdec,
    wz,
    out,
    w_all,
    slots,
    raw,
    state,
    state_in,
    state_out,
    numer,
    denom,
    ret_buf,
    fox_buf,
    mixed,
    part,
    got,
    local_sem,
    ksend,
    krecv,
    ssend,
    srecv,
    wsend,
    wrecv,
    dsend,
    drecv,
    asend,
    arecv,
    osend,
    orecv,
):
    sp = lax.axis_index("sp")
    tp = lax.axis_index("tp")
    g = lax.rem(sp, group)
    z = sp // group
    depth = n_sp // group
    hret = rq.shape[0]
    hfox = fq.shape[0]
    run = rq.shape[1]
    tok = run // group
    rows = out.shape[0]
    after = lax.rem(sp + group, n_sp)
    before = lax.rem(sp + n_sp - group, n_sp)
    f32 = jnp.float32

    def peer(other):
        return z * group + other

    barrier = pltpu.get_barrier_semaphore()
    for i in range(1, group):
        pl.semaphore_signal(
            barrier, inc=1, device_id=(peer(lax.rem(g + i, group)), tp), device_id_type=MESH
        )
    for i in range(1, n_tp):
        pl.semaphore_signal(
            barrier, inc=1, device_id=(sp, lax.rem(tp + i, n_tp)), device_id_type=MESH
        )
    if depth > 1:

        @pl.when(z < depth - 1)
        def _():
            pl.semaphore_signal(barrier, inc=1, device_id=(after, tp), device_id_type=MESH)

        @pl.when(z > 0)
        def _():
            pl.semaphore_signal(barrier, inc=1, device_id=(before, tp), device_id_type=MESH)

    ends = (z + depth - 1) // depth + (2 * depth - 2 - z) // depth
    pl.semaphore_wait(barrier, group + n_tp - 2 + ends)

    def first_hop():
        return remote(fkv, slots.at[z], ksend.at[z], krecv.at[z], after, tp)

    def hop(block):
        return remote(
            slots.at[block], slots.at[block], ksend.at[block], krecv.at[block], after, tp
        )

    if depth > 1:

        @pl.when(z < depth - 1)
        def _():
            first_hop().start()

    hyper = group == 4
    mine = pltpu.make_async_copy(wz, w_all.at[g], local_sem.at[0])
    mine.start()
    direct = []
    for i in range(1, group):
        if hyper and i == 3:
            continue
        other = lax.bitwise_xor(g, i) if hyper else lax.rem(g + i, group)
        direct.append(
            remote(wz, w_all.at[g], wsend.at[i], wrecv.at[i], peer(other), tp)
        )
    for copy in direct:
        copy.start()

    def relay(i):
        source = lax.bitwise_xor(g, i)
        target = lax.bitwise_xor(g, 3 - i)
        span = pl.ds((i - 1) * (depth // 2), depth // 2)
        return remote(
            w_all.at[source, span],
            w_all.at[source, span],
            dsend.at[i],
            drecv.at[i],
            peer(target),
            tp,
        )

    for h in range(hret):
        state[h] = jnp.zeros(state.shape[1:], f32)

        def ret_step(b, carry):
            span = pl.ds(pl.multiple_of(b * BLOCK, BLOCK), BLOCK)
            q = rq[h, span, :]
            k = rk[h, span, :]
            v = rv[h, span, :]
            scores = (
                lax.dot_general(q, k, (((1,), (1,)), ((), ())), preferred_element_type=f32)
                * within[h]
            )
            inner = jnp.dot(scores.astype(jnp.bfloat16), v, preferred_element_type=f32)
            held = state[h]
            cross = jnp.dot(q, held.astype(jnp.bfloat16), preferred_element_type=f32)
            raw[h, span, :] = inner + cross * qdec[h, pl.ds(0, BLOCK), :]
            scaled = (k.astype(f32) * kdec[h]).astype(jnp.bfloat16)
            update = lax.dot_general(
                scaled, v, (((0,), (0,)), ((), ())), preferred_element_type=f32
            )
            state[h] = held * bdec[h, 0:1, :] + update
            return carry

        lax.fori_loop(0, run // BLOCK, ret_step, 0)

    def state_hop():
        return remote(state_out, state_in, ssend.at[0], srecv.at[0], after, tp)

    if depth > 1:

        @pl.when(z == 0)
        def _():
            state_out[...] = state[...]
            state_hop().start()

    tile = math.gcd(run, 256)
    inverse = FOX_DIM ** (-0.5)

    def attend(h, t, keys, values, key_gates, diagonal, fresh):
        span = pl.ds(pl.multiple_of(t * tile, tile), tile)
        scores = (
            lax.dot_general(
                fq[h, span, :], keys, (((1,), (1,)), ((), ())), preferred_element_type=f32
            )
            * inverse
        )
        scores = scores + gq[h, span, :] - key_gates
        if diagonal:
            row = lax.broadcasted_iota(jnp.int32, scores.shape, 0)
            col = lax.broadcasted_iota(jnp.int32, scores.shape, 1)
            scores = jnp.where(col <= row, scores, -jnp.inf)
        weights = jnp.exp(scores)
        total = jnp.sum(weights, axis=1, keepdims=True)
        product = jnp.dot(weights.astype(jnp.bfloat16), values, preferred_element_type=f32)
        if fresh:
            numer[h, span, :] = product
            denom[h, span, :] = total
        else:
            numer[h, span, :] += product
            denom[h, span, :] += total

    for h in range(hfox):
        for t in range(run // tile):
            for s in range(t, -1, -1):
                span = pl.ds(s * tile, tile)
                attend(
                    h,
                    t,
                    fkv[0, h, span, :],
                    fkv[1, h, span, :],
                    gk[h, z, :, span],
                    s == t,
                    s == t,
                )

    def carried():
        state_hop().wait_recv()

        @pl.when(z < depth - 1)
        def _():
            for h in range(hret):
                state_out[h] = state_in[h] * bdec[h, 1:2, :] + state[h]
            state_hop().start()

        for h in range(hret):
            held = state_in[h].astype(jnp.bfloat16)

            def cross_step(b, carry):
                span = pl.ds(pl.multiple_of(b * tile, tile), tile)
                cross = jnp.dot(rq[h, span, :], held, preferred_element_type=f32)
                raw[h, span, :] += cross * qdec[h, span, :]
                return carry

            lax.fori_loop(0, run // tile, cross_step, 0)

    def earlier(step, carry):
        @pl.when(step <= z)
        def _():
            block = z - step
            hop(block).wait_recv()

            @pl.when(z < depth - 1)
            def _():
                hop(block).start()

            for h in range(hfox):

                def query_step(t, c):
                    attend(
                        h,
                        t,
                        slots[block, 0, h],
                        slots[block, 1, h],
                        gk[h, block],
                        False,
                        False,
                    )
                    return c

                lax.fori_loop(0, run // tile, query_step, 0)

        return carry

    if depth > 1:
        lax.fori_loop(1, 2, earlier, 0)

        @pl.when(z > 0)
        def _():
            carried()

        if hyper:
            direct[0].wait_recv()
            relay(1).start()
            direct[1].wait_recv()
            relay(2).start()
        lax.fori_loop(2, depth, earlier, 0)
    elif hyper:
        direct[0].wait_recv()
        relay(1).start()
        direct[1].wait_recv()
        relay(2).start()

    rw = hret * RET_DIM
    fw = hfox * FOX_DIM
    for t in range(group):
        span = pl.ds(t * tok, tok)
        for h in range(hret):
            ret_buf[t, :, h * RET_DIM : (h + 1) * RET_DIM] = normalize(raw[h, span, :])
        for h in range(hfox):
            fox_buf[t, :, h * FOX_DIM : (h + 1) * FOX_DIM] = normalize(
                numer[h, span, :] / denom[h, span, :]
            )
    ret_cols = pl.ds(pl.multiple_of(g * rw, 128), rw)
    fox_cols = pl.ds(pl.multiple_of(group * rw + g * fw, 128), fw)
    exchange = []
    for i in range(1, group):
        other = lax.rem(g + i, group)
        for kind, (buf, cols) in enumerate(((ret_buf, ret_cols), (fox_buf, fox_cols))):
            copy = remote(
                buf.at[other],
                mixed.at[:, cols],
                asend.at[kind, i],
                arecv.at[kind, i],
                peer(other),
                tp,
            )
            copy.start()
            exchange.append(copy)
    mixed[:, ret_cols] = ret_buf[g]
    mixed[:, fox_cols] = fox_buf[g]
    for copy in exchange:
        copy.wait_recv()
    mine.wait()
    if hyper:
        relay(1).wait_recv()
        relay(2).wait_recv()
    else:
        for copy in direct:
            copy.wait_recv()

    cols = w_all.shape[3]
    pack = max(1, 128 // cols)
    wide = pack * cols
    for t in range(n_tp):
        left = mixed[t * rows : (t + 1) * rows, :]

        def column(p, carry, left=left, t=t):
            blocks = [
                w_all[lax.rem(p * pack + i, group), (p * pack + i) // group]
                for i in range(pack)
            ]
            right = blocks[0] if pack == 1 else jnp.concatenate(blocks, axis=1)
            product = jnp.dot(left, right, preferred_element_type=f32)
            at = pl.ds(pl.multiple_of(p * wide, wide), wide)
            part[t, :, at] = product.astype(jnp.bfloat16)
            return carry

        lax.fori_loop(0, n_sp // pack, column, 0)
    final = []
    for i in range(1, n_tp):
        other = lax.rem(tp + i, n_tp)
        copy = remote(part.at[other], got.at[i], osend.at[i], orecv.at[i], sp, other)
        copy.start()
        final.append(copy)
    total = part[tp].astype(f32)
    for i in range(1, n_tp):
        final[i - 1].wait_recv()
        total = total + got[i].astype(f32)
    out[...] = total.astype(jnp.bfloat16)

    for copy in final + exchange + direct:
        copy.wait_send()
    if hyper:
        relay(1).wait_send()
        relay(2).wait_send()
    if depth > 1:

        @pl.when(z < depth - 1)
        def _():
            first_hop().wait_send()
            state_hop().wait_send()

            def settle(block, carry):
                @pl.when(block < z)
                def _():
                    hop(block).wait_send()

                return carry

            lax.fori_loop(0, depth, settle, 0)


def mixer(rq, rk, rv, fq, fkv, gq, gk, within, qdec, kdec, bdec, wz, rows, n_sp, n_tp, group):
    depth = n_sp // group
    hret, run, _ = rq.shape
    hfox = fq.shape[0]
    tok = run // group
    out_rows, cols = wz.shape[1:]
    width = n_sp * cols
    vmem = pl.BlockSpec(memory_space=pltpu.VMEM)
    dma = pltpu.SemaphoreType.DMA
    f32 = jnp.float32
    bf16 = jnp.bfloat16
    square = (hret, RET_DIM, RET_DIM)
    return pl.pallas_call(
        functools.partial(mixer_kernel, n_sp, n_tp, group),
        out_shape=jax.ShapeDtypeStruct((rows, width), bf16),
        in_specs=[vmem] * 11 + [pl.BlockSpec(memory_space=pl.ANY)],
        out_specs=vmem,
        scratch_shapes=[
            pltpu.VMEM((group,) + wz.shape, bf16),
            pltpu.VMEM((depth,) + fkv.shape, bf16),
            pltpu.VMEM((hret, run, RET_DIM), f32),
            pltpu.VMEM(square, f32),
            pltpu.VMEM(square, f32),
            pltpu.VMEM(square, f32),
            pltpu.VMEM((hfox, run, FOX_DIM), f32),
            pltpu.VMEM((hfox, run, 1), f32),
            pltpu.VMEM((group, tok, hret * RET_DIM), bf16),
            pltpu.VMEM((group, tok, hfox * FOX_DIM), bf16),
            pltpu.VMEM((tok, out_rows), bf16),
            pltpu.VMEM((n_tp, rows, width), bf16),
            pltpu.VMEM((n_tp, rows, width), bf16),
            dma((1,)),
            dma((depth,)),
            dma((depth,)),
            dma((1,)),
            dma((1,)),
            dma((max(group, 2),)),
            dma((max(group, 2),)),
            dma((3,)),
            dma((3,)),
            dma((2, group)),
            dma((2, group)),
            dma((n_tp,)),
            dma((n_tp,)),
        ],
        compiler_params=pltpu.CompilerParams(
            collective_id=1, has_side_effects=True, vmem_limit_bytes=VMEM_LIMIT
        ),
        name="mixer",
    )(rq, rk, rv, fq, fkv, gq, gk, within, qdec, kdec, bdec, wz)


def decay_rates(head_ids, total):
    heads_float = head_ids.astype(jnp.float32)
    middle = RET_HEADS // 2
    fast_rate = 1.0 / (32.0 + 16.0 * heads_float)
    slow_rate = jnp.exp2(-(heads_float - middle)) / total
    return jnp.where(head_ids < middle, fast_rate, slow_rate)


def per_device(
    n_sp,
    n_tp,
    tokens,
    gain,
    w_ret_q,
    w_ret_k,
    w_ret_v,
    w_fox_q,
    w_fox_k,
    w_fox_v,
    fox_gates,
    w_out_ret,
    w_out_fox,
):
    f32 = jnp.float32
    bf16 = jnp.bfloat16
    rows, width = tokens.shape
    ret_heads = w_ret_q.shape[1] // RET_DIM
    fox_heads = w_fox_q.shape[1] // FOX_DIM
    group = math.gcd(math.gcd(ret_heads, fox_heads), n_sp)
    depth = n_sp // group
    hret = ret_heads // group
    hfox = fox_heads // group
    run = rows * n_tp * group
    sp = lax.axis_index("sp")
    g = lax.rem(sp, group)
    z = sp // group

    xall, gall, wz = gather(
        tokens, gain.reshape(1, width), fox_gates.T, w_out_ret, w_out_fox, n_sp, n_tp, group
    )
    x = xall.reshape(run, width)

    def project(matrix, heads, size):
        cut = lax.dynamic_slice_in_dim(matrix, g * heads * size, heads * size, 1)
        return jnp.dot(x, cut, preferred_element_type=f32).astype(bf16)

    def split(values, size):
        return values.reshape(run, -1, size).transpose(1, 0, 2)

    positions = z * run + jnp.arange(run, dtype=jnp.int32)
    half = RET_DIM // 2
    inverse = 10000.0 ** (-jnp.arange(half, dtype=f32) / half)
    angles = positions.astype(f32)[:, None] * inverse[None, :]
    cosine = jnp.cos(angles)[None]
    sine = jnp.sin(angles)[None]

    def rotate(values):
        wide = values.astype(f32)
        a = wide[..., :half]
        b = wide[..., half:]
        return jnp.concatenate([a * cosine - b * sine, a * sine + b * cosine], axis=-1)

    rq = rotate(split(project(w_ret_q, hret, RET_DIM), RET_DIM)).astype(bf16)
    rk = (
        rotate(split(project(w_ret_k, hret, RET_DIM), RET_DIM)) * RET_DIM ** (-0.5)
    ).astype(bf16)
    rv = split(project(w_ret_v, hret, RET_DIM), RET_DIM)
    fq = split(project(w_fox_q, hfox, FOX_DIM), FOX_DIM)
    fk = split(project(w_fox_k, hfox, FOX_DIM), FOX_DIM)
    fv = split(project(w_fox_v, hfox, FOX_DIM), FOX_DIM)
    fkv = jnp.stack([fk, fv])

    head_ids = (
        lax.axis_index("tp") * ret_heads + g * hret + jnp.arange(hret, dtype=jnp.int32)
    )
    rates = decay_rates(head_ids, float(run * depth))
    offsets = jnp.arange(BLOCK, dtype=f32)
    spread = offsets[:, None] - offsets[None, :]
    causal = spread >= 0
    within = jnp.where(
        causal[None], jnp.exp(-rates[:, None, None] * jnp.where(causal, spread, 0.0)[None]), 0.0
    )
    steps = jnp.arange(run, dtype=f32)
    qdec = jnp.exp(-rates[:, None] * (steps[None, :] + 1.0))[:, :, None]
    kdec = jnp.exp(-rates[:, None] * (BLOCK - 1.0 - offsets[None, :]))[:, :, None]
    lengths = jnp.array([BLOCK, run], f32)
    bdec = jnp.broadcast_to(
        jnp.exp(-rates[:, None] * lengths[None, :])[:, :, None], (hret, 2, RET_DIM)
    )

    own_gates = lax.dynamic_slice_in_dim(gall, g * hfox, hfox, 1)
    line = own_gates.transpose(1, 0, 2).reshape(hfox, depth, 1, run)
    gq = lax.dynamic_index_in_dim(line, z, 1, False).reshape(hfox, run, 1)
    return mixer(
        rq, rk, rv, fq, fkv, gq, line, within, qdec, kdec, bdec, wz, rows, n_sp, n_tp, group
    )


def solution(mesh):
    in_specs = (
        P(("sp", "tp"), None),
        P(),
        P(None, "tp"),
        P(None, "tp"),
        P(None, "tp"),
        P(None, "tp"),
        P(None, "tp"),
        P(None, "tp"),
        P("sp", "tp"),
        P("tp", "sp"),
        P("tp", "sp"),
    )
    out_specs = P(("sp", "tp"), None)
    return jax.shard_map(
        functools.partial(per_device, mesh.shape["sp"], mesh.shape["tp"]),
        mesh=mesh,
        in_specs=in_specs,
        out_specs=out_specs,
        check_vma=False,
    )
```

```python
import functools
import math

import jax
import jax.numpy as jnp
from jax import lax
from jax.experimental import pallas as pl
from jax.experimental.pallas import tpu as pltpu
from jax.sharding import PartitionSpec as P

RET_HEADS = 8
RET_DIM = 256
FOX_DIM = 128
BLOCK = 128
MESH = pl.DeviceIdType.MESH
VMEM_LIMIT = 60 * 1024 * 1024

eps = 1e-06


def remote(src, dst, send, recv, sp, tp):
    return pltpu.make_async_remote_copy(
        src_ref=src,
        dst_ref=dst,
        send_sem=send,
        recv_sem=recv,
        device_id=(sp, tp),
        device_id_type=MESH,
    )


def gather_kernel(
    n_sp,
    n_tp,
    group,
    tok_ref,
    gain_ref,
    gates_ref,
    wr_ref,
    wf_ref,
    cos_ref,
    sin_ref,
    w_in,
    rq,
    rk,
    rv,
    fq,
    fkv,
    gall,
    wz,
    own,
    xall,
    w_ret,
    w_fox,
    local_sem,
    in_sem,
    tsend,
    trecv,
    dsend,
    drecv,
    psend,
    precv,
    gsend,
    grecv,
    usend,
    urecv,
    nsend,
    nrecv,
):
    sp = lax.axis_index("sp")
    tp = lax.axis_index("tp")
    g = lax.rem(sp, group)
    z = sp // group
    depth = n_sp // group
    rows = tok_ref.shape[0]
    half = rows // 2
    krows = wr_ref.shape[0]

    barrier = pltpu.get_barrier_semaphore()
    for i in range(1, n_sp):
        pl.semaphore_signal(
            barrier, inc=1, device_id=(lax.rem(sp + i, n_sp), tp), device_id_type=MESH
        )
    for i in range(1, n_tp):
        pl.semaphore_signal(
            barrier, inc=1, device_id=(sp, lax.rem(tp + i, n_tp)), device_id_type=MESH
        )

    loads = []
    for i in range(6):
        cut = w_ret if i < 3 else w_fox
        size = cut.shape[2]
        columns = pl.ds(pl.multiple_of(g * size, 128), size)
        loads.append(
            pltpu.make_async_copy(w_in[i].at[:, columns], cut.at[i % 3], in_sem.at[i])
        )

    values = tok_ref[...].astype(jnp.float32)
    scale = lax.rsqrt(jnp.mean(values * values, axis=1, keepdims=True) + eps)
    own[...] = (values * scale * gain_ref[...]).astype(jnp.bfloat16)
    copies = [
        pltpu.make_async_copy(wr_ref, wz.at[z, pl.ds(0, krows)], local_sem.at[0]),
        pltpu.make_async_copy(
            wf_ref, wz.at[z, pl.ds(krows, wf_ref.shape[0])], local_sem.at[1]
        ),
        pltpu.make_async_copy(gates_ref, gall.at[sp], local_sem.at[2]),
    ]
    for copy in copies + loads:
        copy.start()
    pl.semaphore_wait(barrier, n_sp + n_tp - 2)

    def slot(which, core):
        return xall.at[which * n_tp + core]

    mine = pltpu.make_async_copy(own, slot(g, tp), local_sem.at[3])
    mine.start()

    def peer(other):
        return z * group + other

    hyper = group == 4
    direct = []
    for i in range(1, group):
        if hyper and i == 3:
            continue
        other = lax.bitwise_xor(g, i) if hyper else lax.rem(g + i, group)
        direct.append(
            remote(own, slot(g, tp), tsend.at[i], trecv.at[i], peer(other), tp)
        )
    for copy in direct:
        copy.start()
    pair = []
    for i in range(1, n_tp):
        copy = remote(
            own, slot(g, tp), psend.at[0, i], precv.at[0, i], sp, lax.rem(tp + i, n_tp)
        )
        copy.start()
        pair.append(copy)
    gate_copies = []
    for i in range(1, n_sp):
        copy = remote(
            gates_ref, gall.at[sp], gsend.at[i], grecv.at[i], lax.rem(sp + i, n_sp), tp
        )
        copy.start()
        gate_copies.append(copy)

    copies[0].wait()
    copies[1].wait()

    def up(block):
        return remote(
            wz.at[block],
            wz.at[block],
            usend.at[block],
            urecv.at[block],
            lax.rem(sp + group, n_sp),
            tp,
        )

    def down(block):
        return remote(
            wz.at[block],
            wz.at[block],
            nsend.at[block],
            nrecv.at[block],
            lax.rem(sp + n_sp - group, n_sp),
            tp,
        )

    @pl.when(z < depth - 1)
    def _():
        up(z).start()

    @pl.when(z > 0)
    def _():
        down(z).start()

    ready = {0: pair[:]}

    def forward(which, row):
        ready[row] = []
        for i in range(1, n_tp):
            copy = remote(
                slot(which, tp),
                slot(which, tp),
                psend.at[row, i],
                precv.at[row, i],
                sp,
                lax.rem(tp + i, n_tp),
            )
            copy.start()
            pair.append(copy)
            ready[row].append(copy)

    count = n_tp * rows
    half_head = RET_DIM // 2

    def project(which, row):
        for copy in ready[row]:
            copy.wait_recv()
        x = xall[pl.ds(which * n_tp, n_tp)].reshape(count, xall.shape[2])
        span = pl.ds(pl.multiple_of(which * count, count), count)
        for i in range(6):
            cut = w_ret if i < 3 else w_fox
            y = jnp.dot(x, cut[i % 3], preferred_element_type=jnp.float32)
            y = y.astype(jnp.bfloat16)
            if i < 2:
                cosine = cos_ref[span, :]
                sine = sin_ref[span, :]
            for h in range(rq.shape[0] if i < 3 else fq.shape[0]):
                if i < 2:
                    lo = h * RET_DIM
                    a = y[:, lo : lo + half_head].astype(jnp.float32)
                    b = y[:, lo + half_head : lo + RET_DIM].astype(jnp.float32)
                    to = rq if i == 0 else rk
                    by = 1.0 if i == 0 else RET_DIM ** (-0.5)
                    first = (a * cosine - b * sine) * by
                    second = (a * sine + b * cosine) * by
                    to[h, span, :half_head] = first.astype(jnp.bfloat16)
                    to[h, span, half_head:] = second.astype(jnp.bfloat16)
                elif i == 2:
                    rv[h, span, :] = y[:, h * RET_DIM : (h + 1) * RET_DIM]
                elif i == 3:
                    fq[h, span, :] = y[:, h * FOX_DIM : (h + 1) * FOX_DIM]
                else:
                    fkv[i - 4, h, span, :] = y[:, h * FOX_DIM : (h + 1) * FOX_DIM]

    mine.wait()
    for copy in loads:
        copy.wait()
    if not hyper:
        project(g, 0)

    if hyper:
        relays = []
        for i in (1, 2):
            direct[i - 1].wait_recv()
            source = lax.bitwise_xor(g, i)
            target = lax.bitwise_xor(g, 3 - i)
            part = pl.ds((i - 1) * half, half)
            copy = remote(
                slot(source, tp).at[part],
                slot(source, tp).at[part],
                dsend.at[i],
                drecv.at[i],
                peer(target),
                tp,
            )
            copy.start()
            relays.append(copy)
            forward(source, i)
        project(g, 0)
    else:
        for i in range(1, group):
            direct[i - 1].wait_recv()
            forward(lax.rem(g + group - i, group), i)
            project(lax.rem(g + group - i, group), i)

    def line(step, carry):
        below = z - step
        above = z + step

        @pl.when(below >= 0)
        def _():
            up(below).wait_recv()

            @pl.when(z < depth - 1)
            def _():
                up(below).start()

        @pl.when(above <= depth - 1)
        def _():
            down(above).wait_recv()

            @pl.when(z > 0)
            def _():
                down(above).start()

        return carry

    split = depth // 2 if hyper else depth
    lax.fori_loop(1, split, line, 0)
    if hyper:
        project(lax.bitwise_xor(g, 1), 1)
        for copy in relays:
            copy.wait_recv()
        forward(lax.bitwise_xor(g, 3), 3)
    lax.fori_loop(split, depth - 1, line, 0)
    if hyper:
        project(lax.bitwise_xor(g, 2), 2)
        project(lax.bitwise_xor(g, 3), 3)
    lax.fori_loop(max(split, depth - 1), depth, line, 0)

    def settle(step, carry):
        @pl.when((z < depth - 1) & (step <= z))
        def _():
            up(step).wait_send()

        @pl.when((z > 0) & (step >= z))
        def _():
            down(step).wait_send()

        return carry

    lax.fori_loop(0, depth, settle, 0)
    for copy in direct:
        copy.wait_send()
    if hyper:
        for copy in relays:
            copy.wait_send()
    for copy in gate_copies:
        copy.wait()
    for copy in pair:
        copy.wait_send()
    copies[2].wait()


def gather(
    tokens, gain, gates, w_ret, w_fox, cosine, sine, w_in, hret, hfox, n_sp, n_tp, group
):
    rows, width = tokens.shape
    depth = n_sp // group
    out_rows = w_ret.shape[0] + w_fox.shape[0]
    vmem = pl.BlockSpec(memory_space=pltpu.VMEM)
    hbm = pl.BlockSpec(memory_space=pl.ANY)
    dma = pltpu.SemaphoreType.DMA
    run = rows * n_tp * group
    bf16 = jnp.bfloat16

    def body(*refs):
        gather_kernel(n_sp, n_tp, group, *refs[:7], refs[7:13], *refs[13:])

    return pl.pallas_call(
        body,
        out_shape=(
            jax.ShapeDtypeStruct((hret, run, RET_DIM), bf16),
            jax.ShapeDtypeStruct((hret, run, RET_DIM), bf16),
            jax.ShapeDtypeStruct((hret, run, RET_DIM), bf16),
            jax.ShapeDtypeStruct((hfox, run, FOX_DIM), bf16),
            jax.ShapeDtypeStruct((2, hfox, run, FOX_DIM), bf16),
            jax.ShapeDtypeStruct((n_sp,) + gates.shape, jnp.float32),
            jax.ShapeDtypeStruct((depth, out_rows, w_ret.shape[1]), jnp.bfloat16),
        ),
        in_specs=[vmem, vmem, vmem, hbm, hbm, vmem, vmem] + [hbm] * 6,
        out_specs=(vmem,) * 7,
        scratch_shapes=[
            pltpu.VMEM((rows, width), bf16),
            pltpu.VMEM((group * n_tp, rows, width), bf16),
            pltpu.VMEM((3, width, hret * RET_DIM), bf16),
            pltpu.VMEM((3, width, hfox * FOX_DIM), bf16),
            dma((4,)),
            dma((6,)),
            dma((max(group, 2),)),
            dma((max(group, 2),)),
            dma((3,)),
            dma((3,)),
            dma((group, n_tp)),
            dma((group, n_tp)),
            dma((n_sp,)),
            dma((n_sp,)),
            dma((depth,)),
            dma((depth,)),
            dma((depth,)),
            dma((depth,)),
        ],
        compiler_params=pltpu.CompilerParams(
            collective_id=0, has_side_effects=True, vmem_limit_bytes=VMEM_LIMIT
        ),
        name="gather",
    )(tokens, gain, gates, w_ret, w_fox, cosine, sine, *w_in)


def normalize(values):
    return (
        values * lax.rsqrt(jnp.mean(values * values, axis=1, keepdims=True) + eps)
    ).astype(jnp.bfloat16)


def mixer_kernel(
    n_sp,
    n_tp,
    group,
    rq,
    rk,
    rv,
    fq,
    fkv,
    gq,
    gk,
    within,
    qdec,
    kdec,
    bdec,
    wz,
    out,
    w_all,
    slots,
    raw,
    state,
    state_in,
    state_out,
    numer,
    denom,
    ret_buf,
    fox_buf,
    mixed,
    part,
    got,
    local_sem,
    ksend,
    krecv,
    ssend,
    srecv,
    wsend,
    wrecv,
    dsend,
    drecv,
    asend,
    arecv,
    osend,
    orecv,
):
    sp = lax.axis_index("sp")
    tp = lax.axis_index("tp")
    g = lax.rem(sp, group)
    z = sp // group
    depth = n_sp // group
    hret = rq.shape[0]
    hfox = fq.shape[0]
    run = rq.shape[1]
    tok = run // group
    rows = out.shape[0]
    after = lax.rem(sp + group, n_sp)
    before = lax.rem(sp + n_sp - group, n_sp)
    f32 = jnp.float32

    def peer(other):
        return z * group + other

    barrier = pltpu.get_barrier_semaphore()
    for i in range(1, group):
        pl.semaphore_signal(
            barrier, inc=1, device_id=(peer(lax.rem(g + i, group)), tp), device_id_type=MESH
        )
    for i in range(1, n_tp):
        pl.semaphore_signal(
            barrier, inc=1, device_id=(sp, lax.rem(tp + i, n_tp)), device_id_type=MESH
        )
    if depth > 1:

        @pl.when(z < depth - 1)
        def _():
            pl.semaphore_signal(barrier, inc=1, device_id=(after, tp), device_id_type=MESH)

        @pl.when(z > 0)
        def _():
            pl.semaphore_signal(barrier, inc=1, device_id=(before, tp), device_id_type=MESH)

    ends = (z + depth - 1) // depth + (2 * depth - 2 - z) // depth
    pl.semaphore_wait(barrier, group + n_tp - 2 + ends)

    def first_hop():
        return remote(fkv, slots.at[z], ksend.at[z], krecv.at[z], after, tp)

    def hop(block):
        return remote(
            slots.at[block], slots.at[block], ksend.at[block], krecv.at[block], after, tp
        )

    if depth > 1:

        @pl.when(z < depth - 1)
        def _():
            first_hop().start()

    hyper = group == 4
    mine = pltpu.make_async_copy(wz, w_all.at[g], local_sem.at[0])
    mine.start()
    direct = []
    for i in range(1, group):
        if hyper and i == 3:
            continue
        other = lax.bitwise_xor(g, i) if hyper else lax.rem(g + i, group)
        direct.append(
            remote(wz, w_all.at[g], wsend.at[i], wrecv.at[i], peer(other), tp)
        )
    for copy in direct:
        copy.start()

    def relay(i):
        source = lax.bitwise_xor(g, i)
        target = lax.bitwise_xor(g, 3 - i)
        span = pl.ds((i - 1) * (depth // 2), depth // 2)
        return remote(
            w_all.at[source, span],
            w_all.at[source, span],
            dsend.at[i],
            drecv.at[i],
            peer(target),
            tp,
        )

    for h in range(hret):
        state[h] = jnp.zeros(state.shape[1:], f32)

        def ret_step(b, carry):
            span = pl.ds(pl.multiple_of(b * BLOCK, BLOCK), BLOCK)
            q = rq[h, span, :]
            k = rk[h, span, :]
            v = rv[h, span, :]
            scores = (
                lax.dot_general(q, k, (((1,), (1,)), ((), ())), preferred_element_type=f32)
                * within[h]
            )
            inner = jnp.dot(scores.astype(jnp.bfloat16), v, preferred_element_type=f32)
            held = state[h]
            cross = jnp.dot(q, held.astype(jnp.bfloat16), preferred_element_type=f32)
            raw[h, span, :] = inner + cross * qdec[h, pl.ds(0, BLOCK), :]
            scaled = (k.astype(f32) * kdec[h]).astype(jnp.bfloat16)
            update = lax.dot_general(
                scaled, v, (((0,), (0,)), ((), ())), preferred_element_type=f32
            )
            state[h] = held * bdec[h, 0:1, :] + update
            return carry

        lax.fori_loop(0, run // BLOCK, ret_step, 0)

    def state_hop():
        return remote(state_out, state_in, ssend.at[0], srecv.at[0], after, tp)

    if depth > 1:

        @pl.when(z == 0)
        def _():
            state_out[...] = state[...]
            state_hop().start()

    tile = math.gcd(run, 256)
    inverse = FOX_DIM ** (-0.5)

    def attend(h, t, keys, values, key_gates, diagonal, fresh):
        span = pl.ds(pl.multiple_of(t * tile, tile), tile)
        scores = (
            lax.dot_general(
                fq[h, span, :], keys, (((1,), (1,)), ((), ())), preferred_element_type=f32
            )
            * inverse
        )
        scores = scores + gq[h, span, :] - key_gates
        if diagonal:
            row = lax.broadcasted_iota(jnp.int32, scores.shape, 0)
            col = lax.broadcasted_iota(jnp.int32, scores.shape, 1)
            scores = jnp.where(col <= row, scores, -jnp.inf)
        weights = jnp.exp(scores)
        total = jnp.sum(weights, axis=1, keepdims=True)
        product = jnp.dot(weights.astype(jnp.bfloat16), values, preferred_element_type=f32)
        if fresh:
            numer[h, span, :] = product
            denom[h, span, :] = total
        else:
            numer[h, span, :] += product
            denom[h, span, :] += total

    for h in range(hfox):
        for t in range(run // tile):
            for s in range(t, -1, -1):
                span = pl.ds(s * tile, tile)
                attend(
                    h,
                    t,
                    fkv[0, h, span, :],
                    fkv[1, h, span, :],
                    gk[h, z, :, span],
                    s == t,
                    s == t,
                )

    def carried():
        state_hop().wait_recv()

        @pl.when(z < depth - 1)
        def _():
            for h in range(hret):
                state_out[h] = state_in[h] * bdec[h, 1:2, :] + state[h]
            state_hop().start()

        for h in range(hret):
            held = state_in[h].astype(jnp.bfloat16)

            def cross_step(b, carry):
                span = pl.ds(pl.multiple_of(b * tile, tile), tile)
                cross = jnp.dot(rq[h, span, :], held, preferred_element_type=f32)
                raw[h, span, :] += cross * qdec[h, span, :]
                return carry

            lax.fori_loop(0, run // tile, cross_step, 0)

    def earlier(step, carry):
        @pl.when(step <= z)
        def _():
            block = z - step
            hop(block).wait_recv()

            @pl.when(z < depth - 1)
            def _():
                hop(block).start()

            for h in range(hfox):

                def query_step(t, c):
                    attend(
                        h,
                        t,
                        slots[block, 0, h],
                        slots[block, 1, h],
                        gk[h, block],
                        False,
                        False,
                    )
                    return c

                lax.fori_loop(0, run // tile, query_step, 0)

        return carry

    if depth > 1:
        lax.fori_loop(1, 2, earlier, 0)

        @pl.when(z > 0)
        def _():
            carried()

        if hyper:
            direct[0].wait_recv()
            relay(1).start()
            direct[1].wait_recv()
            relay(2).start()
        lax.fori_loop(2, depth, earlier, 0)
    elif hyper:
        direct[0].wait_recv()
        relay(1).start()
        direct[1].wait_recv()
        relay(2).start()

    rw = hret * RET_DIM
    fw = hfox * FOX_DIM
    for t in range(group):
        span = pl.ds(t * tok, tok)
        for h in range(hret):
            ret_buf[t, :, h * RET_DIM : (h + 1) * RET_DIM] = normalize(raw[h, span, :])
        for h in range(hfox):
            fox_buf[t, :, h * FOX_DIM : (h + 1) * FOX_DIM] = normalize(
                numer[h, span, :] / denom[h, span, :]
            )
    ret_cols = pl.ds(pl.multiple_of(g * rw, 128), rw)
    fox_cols = pl.ds(pl.multiple_of(group * rw + g * fw, 128), fw)
    exchange = []
    for i in range(1, group):
        other = lax.rem(g + i, group)
        for kind, (buf, cols) in enumerate(((ret_buf, ret_cols), (fox_buf, fox_cols))):
            copy = remote(
                buf.at[other],
                mixed.at[:, cols],
                asend.at[kind, i],
                arecv.at[kind, i],
                peer(other),
                tp,
            )
            copy.start()
            exchange.append(copy)
    mixed[:, ret_cols] = ret_buf[g]
    mixed[:, fox_cols] = fox_buf[g]
    for copy in exchange:
        copy.wait_recv()
    mine.wait()
    if hyper:
        relay(1).wait_recv()
        relay(2).wait_recv()
    else:
        for copy in direct:
            copy.wait_recv()

    cols = w_all.shape[3]
    pack = max(1, 128 // cols)
    wide = pack * cols
    for t in range(n_tp):
        left = mixed[t * rows : (t + 1) * rows, :]

        def column(p, carry, left=left, t=t):
            blocks = [
                w_all[lax.rem(p * pack + i, group), (p * pack + i) // group]
                for i in range(pack)
            ]
            right = blocks[0] if pack == 1 else jnp.concatenate(blocks, axis=1)
            product = jnp.dot(left, right, preferred_element_type=f32)
            at = pl.ds(pl.multiple_of(p * wide, wide), wide)
            part[t, :, at] = product.astype(jnp.bfloat16)
            return carry

        lax.fori_loop(0, n_sp // pack, column, 0)
    final = []
    for i in range(1, n_tp):
        other = lax.rem(tp + i, n_tp)
        copy = remote(part.at[other], got.at[i], osend.at[i], orecv.at[i], sp, other)
        copy.start()
        final.append(copy)
    total = part[tp].astype(f32)
    for i in range(1, n_tp):
        final[i - 1].wait_recv()
        total = total + got[i].astype(f32)
    out[...] = total.astype(jnp.bfloat16)

    for copy in final + exchange + direct:
        copy.wait_send()
    if hyper:
        relay(1).wait_send()
        relay(2).wait_send()
    if depth > 1:

        @pl.when(z < depth - 1)
        def _():
            first_hop().wait_send()
            state_hop().wait_send()

            def settle(block, carry):
                @pl.when(block < z)
                def _():
                    hop(block).wait_send()

                return carry

            lax.fori_loop(0, depth, settle, 0)


def mixer(rq, rk, rv, fq, fkv, gq, gk, within, qdec, kdec, bdec, wz, rows, n_sp, n_tp, group):
    depth = n_sp // group
    hret, run, _ = rq.shape
    hfox = fq.shape[0]
    tok = run // group
    out_rows, cols = wz.shape[1:]
    width = n_sp * cols
    vmem = pl.BlockSpec(memory_space=pltpu.VMEM)
    dma = pltpu.SemaphoreType.DMA
    f32 = jnp.float32
    bf16 = jnp.bfloat16
    square = (hret, RET_DIM, RET_DIM)
    return pl.pallas_call(
        functools.partial(mixer_kernel, n_sp, n_tp, group),
        out_shape=jax.ShapeDtypeStruct((rows, width), bf16),
        in_specs=[vmem] * 11 + [pl.BlockSpec(memory_space=pl.ANY)],
        out_specs=vmem,
        scratch_shapes=[
            pltpu.VMEM((group,) + wz.shape, bf16),
            pltpu.VMEM((depth,) + fkv.shape, bf16),
            pltpu.VMEM((hret, run, RET_DIM), f32),
            pltpu.VMEM(square, f32),
            pltpu.VMEM(square, f32),
            pltpu.VMEM(square, f32),
            pltpu.VMEM((hfox, run, FOX_DIM), f32),
            pltpu.VMEM((hfox, run, 1), f32),
            pltpu.VMEM((group, tok, hret * RET_DIM), bf16),
            pltpu.VMEM((group, tok, hfox * FOX_DIM), bf16),
            pltpu.VMEM((tok, out_rows), bf16),
            pltpu.VMEM((n_tp, rows, width), bf16),
            pltpu.VMEM((n_tp, rows, width), bf16),
            dma((1,)),
            dma((depth,)),
            dma((depth,)),
            dma((1,)),
            dma((1,)),
            dma((max(group, 2),)),
            dma((max(group, 2),)),
            dma((3,)),
            dma((3,)),
            dma((2, group)),
            dma((2, group)),
            dma((n_tp,)),
            dma((n_tp,)),
        ],
        compiler_params=pltpu.CompilerParams(
            collective_id=1, has_side_effects=True, vmem_limit_bytes=VMEM_LIMIT
        ),
        name="mixer",
    )(rq, rk, rv, fq, fkv, gq, gk, within, qdec, kdec, bdec, wz)


def decay_rates(head_ids, total):
    heads_float = head_ids.astype(jnp.float32)
    middle = RET_HEADS // 2
    fast_rate = 1.0 / (32.0 + 16.0 * heads_float)
    slow_rate = jnp.exp2(-(heads_float - middle)) / total
    return jnp.where(head_ids < middle, fast_rate, slow_rate)


def per_device(
    n_sp,
    n_tp,
    tokens,
    gain,
    w_ret_q,
    w_ret_k,
    w_ret_v,
    w_fox_q,
    w_fox_k,
    w_fox_v,
    fox_gates,
    w_out_ret,
    w_out_fox,
):
    f32 = jnp.float32
    rows, width = tokens.shape
    ret_heads = w_ret_q.shape[1] // RET_DIM
    fox_heads = w_fox_q.shape[1] // FOX_DIM
    group = math.gcd(math.gcd(ret_heads, fox_heads), n_sp)
    depth = n_sp // group
    hret = ret_heads // group
    hfox = fox_heads // group
    run = rows * n_tp * group
    sp = lax.axis_index("sp")
    g = lax.rem(sp, group)
    z = sp // group

    positions = z * run + jnp.arange(run, dtype=jnp.int32)
    half = RET_DIM // 2
    inverse = 10000.0 ** (-jnp.arange(half, dtype=f32) / half)
    angles = positions.astype(f32)[:, None] * inverse[None, :]
    rq, rk, rv, fq, fkv, gall, wz = gather(
        tokens,
        gain.reshape(1, width),
        fox_gates.T,
        w_out_ret,
        w_out_fox,
        jnp.cos(angles),
        jnp.sin(angles),
        (w_ret_q, w_ret_k, w_ret_v, w_fox_q, w_fox_k, w_fox_v),
        hret,
        hfox,
        n_sp,
        n_tp,
        group,
    )

    head_ids = (
        lax.axis_index("tp") * ret_heads + g * hret + jnp.arange(hret, dtype=jnp.int32)
    )
    rates = decay_rates(head_ids, float(run * depth))
    offsets = jnp.arange(BLOCK, dtype=f32)
    spread = offsets[:, None] - offsets[None, :]
    causal = spread >= 0
    within = jnp.where(
        causal[None], jnp.exp(-rates[:, None, None] * jnp.where(causal, spread, 0.0)[None]), 0.0
    )
    steps = jnp.arange(run, dtype=f32)
    qdec = jnp.exp(-rates[:, None] * (steps[None, :] + 1.0))[:, :, None]
    kdec = jnp.exp(-rates[:, None] * (BLOCK - 1.0 - offsets[None, :]))[:, :, None]
    lengths = jnp.array([BLOCK, run], f32)
    bdec = jnp.broadcast_to(
        jnp.exp(-rates[:, None] * lengths[None, :])[:, :, None], (hret, 2, RET_DIM)
    )

    own_gates = lax.dynamic_slice_in_dim(gall, g * hfox, hfox, 1)
    line = own_gates.transpose(1, 0, 2).reshape(hfox, depth, 1, run)
    gq = lax.dynamic_index_in_dim(line, z, 1, False).reshape(hfox, run, 1)
    return mixer(
        rq, rk, rv, fq, fkv, gq, line, within, qdec, kdec, bdec, wz, rows, n_sp, n_tp, group
    )


def solution(mesh):
    in_specs = (
        P(("sp", "tp"), None),
        P(),
        P(None, "tp"),
        P(None, "tp"),
        P(None, "tp"),
        P(None, "tp"),
        P(None, "tp"),
        P(None, "tp"),
        P("sp", "tp"),
        P("tp", "sp"),
        P("tp", "sp"),
    )
    out_specs = P(("sp", "tp"), None)
    return jax.shard_map(
        functools.partial(per_device, mesh.shape["sp"], mesh.shape["tp"]),
        mesh=mesh,
        in_specs=in_specs,
        out_specs=out_specs,
        check_vma=False,
    )
```
